32 devices in a mesh: tp: 8 (over z, y), dp: 4 (over x, core).
Axes of the slice: x: 2, y: 2, z: 4, core: 2. Of those that a mesh axis runs over, the one named last changes fastest.
Arguments:
- tokens: bfloat16 [192, 8448], P('dp', 'tp'), may hold values from -6 to 6
- gains: float32 [2, 8448], replicated, may hold values from 0.1 to 1.9
- w_input: bfloat16 [2, 8448, 12288], P(None, 'dp', 'tp'), may hold values from -0.0625 to 0.0625
- w_gating: bfloat16 [2, 8448, 12288], P(None, 'dp', 'tp'), may hold values from -0.0625 to 0.0625
- w_output: bfloat16 [2, 12288, 8448], P(None, 'tp'), may hold values from -0.21875 to 0.21875
- decay_rate: float32 [2, 768, 64], P(None, 'tp'), may hold values from 0.05 to 2
- frequency: float32 [2, 768, 64], P(None, 'tp'), may hold values from -3 to 3
- log_step: float32 [2, 768], P(None, 'tp'), may hold values from -2.3 to 0
- in_real: float32 [2, 768, 64, 16], P(None, 'tp'), may hold values from -1 to 1
- in_imag: float32 [2, 768, 64, 16], P(None, 'tp'), may hold values from -1 to 1
- readout_real_matrix: float32 [2, 768, 16, 64], P(None, 'tp'), may hold values from -0.5 to 0.5
- readout_imag_matrix: float32 [2, 768, 16, 64], P(None, 'tp'), may hold values from -0.5 to 0.5
- skip_gain: float32 [2, 12288], P(None, 'tp'), may hold values from -4 to 4
- state_real: float32 [2, 192, 768, 64], P(None, 'dp', 'tp'), may hold values from -6 to 6
- state_imag: float32 [2, 192, 768, 64], P(None, 'dp', 'tp'), may hold values from -6 to 6
Outputs:
- mixed: bfloat16 [192, 8448], P('dp', 'tp')
- next_real: float32 [2, 192, 768, 64], P(None, 'dp', 'tp')
- next_imag: float32 [2, 192, 768, 64], P(None, 'dp', 'tp')
The draws below stay inside these ranges and needn't reach their ends.
All inputs are finite; a program needn't handle non-finite values.
Results may differ from the reference program's by a relative error of at most 0.008.
Values may be sent and summed in bfloat16 or wider, within the bound.
A program may use at most 256 MiB of HBM per device.

```python
import math
import jax
import jax.numpy as jnp
from jax import lax

D = 8448
G = 768
GS = 16
P_SIZE = 64
LAYERS = 2
BATCH = 192
W = 12288


def with_spikes(drawn, stream_key, source, target, shards_of, factor):
    owner, partner = [(jnp.arange(drawn.shape[position]) // (drawn.shape[position] // shards_of)).reshape([-1 if axis == position else 1 for axis in range(drawn.ndim)]) for position in (source, target)]
    chosen = jax.random.permutation(stream_key, shards_of)[partner]
    strong = (owner == chosen) | (owner == (partner + shards_of // 2) % shards_of)
    return jnp.where(strong, factor * drawn, drawn)


def steps_of(stream_key, shape, split, low, largest):
    def one(dim, shards_of):
        steps = jax.random.uniform(jax.random.fold_in(jax.random.fold_in(stream_key, 6), dim), (shards_of,), jnp.float32, low / len(split), largest / len(split))
        return jnp.repeat(jnp.exp(steps), shape[dim] // shards_of).reshape((-1,) + (1,) * (len(shape) - dim - 1))

    gain = one(*split[0])
    for cut in split[1:]:
        gain = gain * one(*cut)
    return gain


def gaussian(stream_key, shape, width, bound, pieces=(), dtype=jnp.bfloat16):
    entries = width * jax.random.normal(stream_key, shape, jnp.float32)
    if pieces:
        entries = entries * steps_of(stream_key, shape, pieces, -0.22, 0.18)
    return jnp.clip(entries, -bound, bound).astype(dtype)


def noise_with(rng, dims, width, bound, shards, heavy, kind=jnp.bfloat16):
    entries = width * jax.random.normal(rng, dims, jnp.float32)
    if shards:
        entries = entries * steps_of(rng, dims, shards, -0.22, 0.18)
    return jnp.clip(with_spikes(entries, jax.random.fold_in(rng, 3), *heavy), -bound, bound).astype(kind)


def setup_inputs(seed: int = 0) -> dict:
    streams_of = jax.random.split(jax.random.key(seed), 16)
    return {
        "tokens": gaussian(streams_of[0], (BATCH, D), 1.0, 6.0, ((0, 4), (1, 8))),
        "gains": jnp.clip(1.0 + 0.18 * jax.random.normal(streams_of[1], (LAYERS, D), jnp.float32), 0.1, 1.9),
        "w_input": gaussian(streams_of[2], (LAYERS, D, W), D ** -0.5, 0.0625, ((1, 4), (2, 8))),
        "w_gating": gaussian(streams_of[3], (LAYERS, D, W), D ** -0.5, 0.0625, ((1, 4), (2, 8))),
        "w_output": noise_with(streams_of[4], (LAYERS, W, D), (W // 8) ** -0.5, 0.21875, ((1, 8),), (1, 2, 8, 2.0)),
        "decay_rate": jnp.clip(jnp.exp(math.log(2.0) - 3.6888794 * jax.random.uniform(streams_of[5], (LAYERS, G, P_SIZE), jnp.float32) ** steps_of(streams_of[5], (LAYERS, G, P_SIZE), ((1, 8),), -0.2, 0.2)), 0.05, 2.0),
        "frequency": jnp.clip(jax.random.uniform(streams_of[6], (LAYERS, G, P_SIZE), jnp.float32, -3.0, 3.0) * steps_of(streams_of[6], (LAYERS, G, P_SIZE), ((1, 8),), -0.4, 0.0), -3.0, 3.0),
        "log_step": jnp.clip(-2.3 + 2.3 * jax.random.uniform(streams_of[7], (LAYERS, G), jnp.float32) ** steps_of(streams_of[7], (LAYERS, G), ((1, 8),), -0.2, 0.2), -2.3, 0.0),
        "in_real": gaussian(streams_of[8], (LAYERS, G, P_SIZE, GS), (2 * GS) ** -0.5, 1.0, ((1, 8),), jnp.float32),
        "in_imag": gaussian(streams_of[9], (LAYERS, G, P_SIZE, GS), (2 * GS) ** -0.5, 1.0, ((1, 8),), jnp.float32),
        "readout_real_matrix": gaussian(streams_of[10], (LAYERS, G, GS, P_SIZE), (2 * P_SIZE) ** -0.5, 0.5, ((1, 8),), jnp.float32),
        "readout_imag_matrix": gaussian(streams_of[11], (LAYERS, G, GS, P_SIZE), (2 * P_SIZE) ** -0.5, 0.5, ((1, 8),), jnp.float32),
        "skip_gain": gaussian(streams_of[12], (LAYERS, W), 1.0, 4.0, ((1, 8),), jnp.float32),
        "state_real": gaussian(streams_of[13], (LAYERS, BATCH, G, P_SIZE), 1.0, 6.0, ((1, 4), (2, 8)), jnp.float32),
        "state_imag": gaussian(streams_of[14], (LAYERS, BATCH, G, P_SIZE), 1.0, 6.0, ((1, 4), (2, 8)), jnp.float32),
    }


PRECISION_LEVEL = lax.Precision.HIGHEST

def reference(tokens, gains, w_input, w_gating, w_output, decay_rate, frequency, log_step, in_real, in_imag, readout_real_matrix, readout_imag_matrix, skip_gain, state_real, state_imag):
    x = tokens
    outs_re = []
    outs_im = []
    batch = x.shape[0]
    for layer_params in range(LAYERS):
        xf = x.astype(jnp.float32)
        meansq = lax.optimization_barrier(jnp.mean(xf * xf, axis=1, keepdims=True))
        inverse = lax.rsqrt(meansq + 1e-06)
        scaled = (xf * gains[layer_params][None, :]).astype(jnp.bfloat16)
        drive = jnp.dot(scaled, w_input[layer_params], preferred_element_type=jnp.float32) * inverse
        gate = jnp.dot(scaled, w_gating[layer_params], preferred_element_type=jnp.float32) * inverse
        step = jnp.exp(log_step[layer_params])[:, None]
        lam_re = -decay_rate[layer_params]
        lam_im = frequency[layer_params]
        magnitude = jnp.exp(lam_re * step)
        angle = lam_im * step
        abar_re = magnitude * jnp.cos(angle)
        abar_im = magnitude * jnp.sin(angle)
        denom = lam_re * lam_re + lam_im * lam_im
        num_re = abar_re - 1.0
        zoh_re = (num_re * lam_re + abar_im * lam_im) / denom
        zoh_im = (abar_im * lam_re - num_re * lam_im) / denom
        bbar_re = zoh_re[..., None] * in_real[layer_params] - zoh_im[..., None] * in_imag[layer_params]
        bbar_im = zoh_re[..., None] * in_imag[layer_params] + zoh_im[..., None] * in_real[layer_params]
        grouped = drive.reshape(batch, G, GS)
        push_re = jnp.einsum('bgc,gpc->bgp', grouped, bbar_re, precision=PRECISION_LEVEL)
        push_im = jnp.einsum('bgc,gpc->bgp', grouped, bbar_im, precision=PRECISION_LEVEL)
        old_re = state_real[layer_params]
        old_im = state_imag[layer_params]
        updated_real = abar_re[None] * old_re - abar_im[None] * old_im + push_re
        updated_imag = abar_re[None] * old_im + abar_im[None] * old_re + push_im
        readout_output = jnp.einsum('zju,jiu->zji', updated_real, readout_real_matrix[layer_params], precision=PRECISION_LEVEL) - jnp.einsum('zju,jiu->zji', updated_imag, readout_imag_matrix[layer_params], precision=PRECISION_LEVEL)
        readout_output = readout_output + skip_gain[layer_params].reshape(G, GS)[None] * grouped
        gated = (jax.nn.gelu(readout_output.reshape(batch, G * GS)) * jax.nn.sigmoid(gate)).astype(jnp.bfloat16)
        branch = jnp.dot(gated, w_output[layer_params], preferred_element_type=jnp.float32)
        x = (xf + branch).astype(jnp.bfloat16)
        outs_re.append(updated_real)
        outs_im.append(updated_imag)
    return (x, jnp.stack(outs_re, axis=0), jnp.stack(outs_im, axis=0))
```

```python
import functools

import jax
import jax.numpy as jnp
from jax import lax
from jax.experimental import pallas as pl
from jax.experimental.pallas import tpu as pltpu
from jax.sharding import PartitionSpec as P

GS = 16
LAYERS = 2
MESH = pl.DeviceIdType.MESH
ANY = pl.BlockSpec(memory_space=pl.ANY)


def exchange_kernel(axis, n, count, *refs):
    ins, outs = refs[:count], refs[count : 2 * count]
    send, recv, local = refs[2 * count :]
    me = lax.axis_index(axis)
    barrier = pltpu.get_barrier_semaphore()
    for i in range(1, n):
        pl.semaphore_signal(
            barrier, inc=1, device_id={axis: lax.rem(me + i, n)}, device_id_type=MESH
        )
    own = [
        pltpu.make_async_copy(ins[k].at[me], outs[k].at[me], local.at[k]) for k in range(count)
    ]
    for copy in own:
        copy.start()
    pl.semaphore_wait(barrier, n - 1)
    copies = []
    for i in range(1, n):
        peer = lax.rem(me + i, n)
        for k in range(count):
            copy = pltpu.make_async_remote_copy(
                src_ref=ins[k].at[peer],
                dst_ref=outs[k].at[me],
                send_sem=send.at[k, i],
                recv_sem=recv.at[k, i],
                device_id={axis: peer},
                device_id_type=MESH,
            )
            copy.start()
            copies.append((i, k, copy))
    for copy in own:
        copy.wait()
    for i, k, copy in copies:
        copy.wait_send()
        source = lax.rem(me + n - i, n)
        pltpu.make_async_remote_copy(
            src_ref=ins[k].at[source],
            dst_ref=outs[k].at[source],
            send_sem=send.at[k, i],
            recv_sem=recv.at[k, i],
            device_id={axis: source},
            device_id_type=MESH,
        ).wait_recv()


def exchange(arrays, axis, n, ident):
    count = len(arrays)
    return pl.pallas_call(
        functools.partial(exchange_kernel, axis, n, count),
        out_shape=[jax.ShapeDtypeStruct(a.shape, a.dtype) for a in arrays],
        in_specs=[ANY] * count,
        out_specs=[ANY] * count,
        scratch_shapes=[
            pltpu.SemaphoreType.DMA((count, n)),
            pltpu.SemaphoreType.DMA((count, n)),
            pltpu.SemaphoreType.DMA((count,)),
        ],
        compiler_params=pltpu.CompilerParams(collective_id=ident, has_side_effects=True),
        name=f"exchange_{axis}_{ident}",
    )(*arrays)


def gather_kernel(tp, dp, x_ref, out_ref, send, recv):
    q = tp // dp
    t = lax.axis_index("tp")
    d = lax.axis_index("dp")
    group = t // q
    slot = lax.rem(t, q) * dp + d
    barrier = pltpu.get_barrier_semaphore()
    for h in range(q):
        for r in range(dp):
            source = d * q + h
            pl.semaphore_signal(
                barrier, inc=1, device_id={"tp": source, "dp": r}, device_id_type=MESH
            )

    pl.semaphore_wait(barrier, tp)

    def remote(i, index):
        return pltpu.make_async_remote_copy(
            src_ref=x_ref,
            dst_ref=out_ref.at[index],
            send_sem=send.at[i],
            recv_sem=recv.at[index],
            device_id={"tp": lax.rem(t + i, tp), "dp": group},
            device_id_type=MESH,
        )

    home = group == d

    @pl.when(home)
    def _():
        pltpu.make_async_copy(x_ref, out_ref.at[slot], recv.at[slot]).start()

    @pl.when(jnp.logical_not(home))
    def _():
        remote(0, slot).start()

    for i in range(1, tp):
        remote(i, slot).start()
    for i in range(1, tp):
        remote(i, slot).wait_send()

    @pl.when(jnp.logical_not(home))
    def _():
        remote(0, slot).wait_send()

    for index in range(tp):
        pltpu.make_async_copy(x_ref, out_ref.at[index], recv.at[index]).wait()


def gather(x, tp, dp, ident):
    return pl.pallas_call(
        functools.partial(gather_kernel, tp, dp),
        out_shape=jax.ShapeDtypeStruct((tp,) + x.shape, x.dtype),
        in_specs=[ANY],
        out_specs=ANY,
        scratch_shapes=[pltpu.SemaphoreType.DMA((tp,)), pltpu.SemaphoreType.DMA((tp,))],
        compiler_params=pltpu.CompilerParams(collective_id=ident, has_side_effects=True),
        name=f"gather_{ident}",
    )(x)


def state_kernel(many, u_ref, are_ref, aim_ref, bre_ref, bim_ref, rre_ref, rim_ref, sre_ref, sim_ref, *rest):
    nre_ref, nim_ref, y_ref = rest[-3:]
    block, channels = u_ref.shape[0], u_ref.shape[1]
    states = are_ref.shape[1]
    cut = 4

    def body(step, carry):
        first = step * many
        for p in range(0, states, 8):
            rows = slice(p, p + 8)
            a_re, a_im = are_ref[0, rows, :], aim_ref[0, rows, :]
            new_re, new_im = [], []
            for b in range(many):
                o_re, o_im = sre_ref[0, first + b, rows, :], sim_ref[0, first + b, rows, :]
                new_re.append(a_re * o_re - a_im * o_im)
                new_im.append(a_re * o_im + a_im * o_re)
            for c in range(channels):
                b_re, b_im = bre_ref[0, c, rows, :], bim_ref[0, c, rows, :]
                for b in range(many):
                    u = u_ref[first + b, c : c + 1, :]
                    new_re[b] = new_re[b] + b_re * u
                    new_im[b] = new_im[b] + b_im * u
            for b in range(many):
                nre_ref[0, first + b, rows, :] = new_re[b]
                nim_ref[0, first + b, rows, :] = new_im[b]
        for c in range(0, channels, cut):
            total = [[None] * many for _ in range(cut)]
            for p in range(0, states, 8):
                rows = slice(p, p + 8)
                h_re = [nre_ref[0, first + b, rows, :] for b in range(many)]
                h_im = [nim_ref[0, first + b, rows, :] for b in range(many)]
                for j in range(cut):
                    r_re, r_im = rre_ref[0, c + j, rows, :], rim_ref[0, c + j, rows, :]
                    for b in range(many):
                        term = r_re * h_re[b] - r_im * h_im[b]
                        total[j][b] = term if p == 0 else total[j][b] + term
            for j in range(cut):
                for b in range(many):
                    y_ref[first + b, c + j : c + j + 1, :] = jnp.sum(
                        total[j][b], axis=0, keepdims=True
                    )
        return carry

    lax.fori_loop(0, block // many, body, 0)


def state_step(layer, u, a_re, a_im, b_re, b_im, r_re, r_im, s_re, s_im, earlier):
    batch, channels, groups = u.shape
    states = a_re.shape[1]
    block = 8
    per_batch = pl.BlockSpec((block, channels, groups), lambda i: (i, 0, 0))
    eigen = pl.BlockSpec((1, states, groups), lambda i: (layer, 0, 0))
    matrix = pl.BlockSpec((1, channels, states, groups), lambda i: (layer, 0, 0, 0))
    state = pl.BlockSpec((1, block, states, groups), lambda i: (layer, i, 0, 0))
    specs = [per_batch, eigen, eigen, matrix, matrix, matrix, matrix, state, state]
    aliases = {}
    if earlier:
        aliases = {len(specs): 0, len(specs) + 1: 1}
    return pl.pallas_call(
        functools.partial(state_kernel, 4),
        grid=(batch // block,),
        out_shape=[
            jax.ShapeDtypeStruct(s_re.shape, jnp.float32),
            jax.ShapeDtypeStruct(s_im.shape, jnp.float32),
            jax.ShapeDtypeStruct(u.shape, jnp.float32),
        ],
        in_specs=specs + [ANY] * len(earlier),
        out_specs=[state, state, per_batch],
        input_output_aliases=aliases,
        name=f"state_{layer}",
    )(u, a_re, a_im, b_re, b_im, r_re, r_im, s_re, s_im, *earlier)


def on_device(
    tp,
    dp,
    tokens,
    gains,
    w_input,
    w_gating,
    w_output,
    decay_rate,
    frequency,
    log_step,
    in_real,
    in_imag,
    readout_real_matrix,
    readout_imag_matrix,
    skip_gain,
    state_real,
    state_imag,
):
    batch, width = tokens.shape
    groups, states = decay_rate.shape[1:]
    channels = groups * GS
    rows = w_input.shape[1]
    features = gains.shape[1]
    q = tp // dp
    d = lax.axis_index("dp")

    step = jnp.exp(log_step)[:, None, :]
    lam_re = -jnp.swapaxes(decay_rate, 1, 2)
    lam_im = jnp.swapaxes(frequency, 1, 2)
    magnitude = jnp.exp(lam_re * step)
    angle = lam_im * step
    abar_re = magnitude * jnp.cos(angle)
    abar_im = magnitude * jnp.sin(angle)
    denom = lam_re * lam_re + lam_im * lam_im
    num_re = abar_re - 1.0
    zoh_re = ((num_re * lam_re + abar_im * lam_im) / denom)[:, None]
    zoh_im = ((abar_im * lam_re - num_re * lam_im) / denom)[:, None]
    i_re = jnp.transpose(in_real, (0, 3, 2, 1))
    i_im = jnp.transpose(in_imag, (0, 3, 2, 1))
    bbar_re = zoh_re * i_re - zoh_im * i_im
    bbar_im = zoh_re * i_im + zoh_im * i_re
    r_re = jnp.transpose(readout_real_matrix, (0, 2, 3, 1))
    r_im = jnp.transpose(readout_imag_matrix, (0, 2, 3, 1))
    s_re = jnp.swapaxes(state_real, 2, 3)
    s_im = jnp.swapaxes(state_imag, 2, 3)
    my_gains = lax.dynamic_slice_in_dim(gains, d * rows, rows, 1).reshape(LAYERS, q, 1, width)

    shard = tokens
    news = ()
    for layer in range(LAYERS):
        got = gather(shard, tp, dp, 3 * layer + 1).reshape(q, dp * batch, width)
        xf = got.astype(jnp.float32)
        squares = jnp.sum(xf * xf, axis=(0, 2))
        scaled = (xf * my_gains[layer]).astype(jnp.bfloat16)
        if q <= 2:
            scaled = jnp.concatenate([scaled[h] for h in range(q)], axis=1)
        else:
            scaled = jnp.swapaxes(scaled, 0, 1).reshape(dp * batch, rows)
        drive = jnp.dot(scaled, w_input[layer], preferred_element_type=jnp.float32)
        gate = jnp.dot(scaled, w_gating[layer], preferred_element_type=jnp.float32)
        drive, gate, squares = exchange(
            [
                drive.astype(jnp.bfloat16).reshape(dp, batch, channels),
                gate.astype(jnp.bfloat16).reshape(dp, batch, channels),
                jnp.broadcast_to(squares.reshape(dp, batch, 1), (dp, batch, 128)),
            ],
            "dp",
            dp,
            3 * layer + 2,
        )
        meansq = jnp.sum(squares, axis=0)[:, :1] / features
        inverse = lax.rsqrt(meansq + 1e-06)
        drive = jnp.sum(drive.astype(jnp.float32), axis=0) * inverse
        gate = jnp.sum(gate.astype(jnp.float32), axis=0) * inverse
        u = jnp.swapaxes(drive.reshape(batch, groups, GS), 1, 2)
        n_re, n_im, y = state_step(
            layer, u, abar_re, abar_im, bbar_re, bbar_im, r_re, r_im, s_re, s_im, news
        )
        news = (n_re, n_im)
        y = jnp.swapaxes(y, 1, 2).reshape(batch, channels) + skip_gain[layer][None] * drive
        z = (jax.nn.gelu(y) * jax.nn.sigmoid(gate)).astype(jnp.bfloat16)
        branch = jnp.dot(z, w_output[layer], preferred_element_type=jnp.float32)
        pieces = jnp.swapaxes(branch.astype(jnp.bfloat16).reshape(batch, tp, width), 0, 1)
        (pieces,) = exchange([pieces], "tp", tp, 3 * layer + 3)
        summed = jnp.sum(pieces.astype(jnp.float32), axis=0)
        shard = (shard.astype(jnp.float32) + summed).astype(jnp.bfloat16)
    return shard, jnp.swapaxes(news[0], 2, 3), jnp.swapaxes(news[1], 2, 3)


def solution(mesh):
    placed = (
        P("dp", "tp"),
        P(),
        P(None, "dp", "tp"),
        P(None, "dp", "tp"),
        P(None, "tp", None),
        P(None, "tp", None),
        P(None, "tp", None),
        P(None, "tp"),
        P(None, "tp", None, None),
        P(None, "tp", None, None),
        P(None, "tp", None, None),
        P(None, "tp", None, None),
        P(None, "tp"),
        P(None, "dp", "tp", None),
        P(None, "dp", "tp", None),
    )
    return jax.shard_map(
        functools.partial(on_device, mesh.shape["tp"], mesh.shape["dp"]),
        mesh=mesh,
        in_specs=placed,
        out_specs=(P("dp", "tp"), P(None, "dp", "tp", None), P(None, "dp", "tp", None)),
        check_vma=False,
    )
```
